32 devices in a mesh: kv: 8 (over z, y), tp: 4 (over x, core).
Axes of the slice: x: 2, y: 2, z: 4, core: 2. Of those that a mesh axis runs over, the one named last changes fastest.
Arguments:
- tokens: bfloat16 [16, 4096], P(None, ('kv', 'tp')), may hold values from -6 to 6
- gain_attn: bfloat16 [4096], replicated, may hold values from 0.099609375 to 1.8984375
- w_query: bfloat16 [4096, 2048], P('kv', 'tp'), may hold values from -0.09375 to 0.09375
- w_key: bfloat16 [4096, 2048], P('kv', 'tp'), may hold values from -0.09375 to 0.09375
- w_value: bfloat16 [4096, 2048], P('kv', 'tp'), may hold values from -0.09375 to 0.09375
- w_forget: bfloat16 [4096, 32], replicated, may hold values from -0.09375 to 0.09375
- forget_bias: float32 [32], replicated, may hold values from -2 to 2
- keys_cache: bfloat16 [16, 4096, 2048], P(None, 'kv', 'tp'), may hold values from -900 to 900
- values_cache: bfloat16 [16, 4096, 2048], P(None, 'kv', 'tp'), may hold values from -6 to 6
- gates_cache: float32 [16, 32, 4096], P(None, 'tp', 'kv'), as said below
- lengths: int32 [16], replicated, may hold values from 1 to 4096, 32768 in all
- w_out: bfloat16 [2048, 4096], P('tp', 'kv'), may hold values from -0.1875 to 0.1875
- gain_mixer: bfloat16 [4096], replicated, may hold values from 0.099609375 to 1.8984375
- w_up: bfloat16 [4096, 16384], P('kv', 'tp'), may hold values from -0.09375 to 0.09375
- w_down: bfloat16 [16384, 4096], P('tp', 'kv'), may hold values from -0.0625 to 0.0625
Outputs:
- output: bfloat16 [16, 4096], P(None, ('kv', 'tp'))
The draws below stay inside these ranges and needn't reach their ends.
Inputs may be any that keep to these rules, and one draw needn't show every extreme that they name: One sequence has all 4096 positions live; the lengths add up to half of 16 times 4096. `gates_cache`: along positions each entry is the running sum of per-position log forget gates up to and including that position, so the values never rise.
All inputs are finite; a program needn't handle non-finite values.
Results may differ from the reference program's by a relative error of at most 0.017.
Values may be sent and summed in bfloat16 or wider, within the bound.
A program may use at most 128 MiB of HBM per device.

```python
import math
import jax
import jax.numpy as jnp
import numpy as np
from jax import lax

D = 4096
ATTENDER_NUMBER = 32
FF = 16384
BATCH_STRINGS = 16
STORED_POSITIONS = 4096
QW = 2048
N_KV = 8
N_TP = 4


def draw_gates_cache(key, part):
    split_prng_material = jax.random.split(jax.random.fold_in(key, 7), 6)
    share = 0.5
    slow_heads = jax.random.uniform(split_prng_material[0], (ATTENDER_NUMBER,)) < share
    slow_rate = jnp.exp(jax.random.uniform(split_prng_material[1], (ATTENDER_NUMBER,), minval=jnp.log(0.2), maxval=jnp.log(0.8))) / STORED_POSITIONS
    fast_rate = jnp.exp(jax.random.uniform(split_prng_material[2], (ATTENDER_NUMBER,), minval=jnp.log(0.01), maxval=jnp.log(1.0 / 30.0)))
    rate = jnp.where(slow_heads, slow_rate, fast_rate)
    factor = jnp.exp(jax.random.uniform(split_prng_material[3], (BATCH_STRINGS, ATTENDER_NUMBER, N_KV), minval=-0.7, maxval=0.7))
    factor = jnp.repeat(factor, STORED_POSITIONS // N_KV, axis=-1)
    rough = jax.random.uniform(split_prng_material[4], (BATCH_STRINGS, ATTENDER_NUMBER, STORED_POSITIONS), minval=0.5, maxval=1.5)
    decoding_logarithmic_decays = -rate[None, :, None] * factor * rough
    draw_filled_extents = jax.random.uniform(split_prng_material[5], (2, BATCH_STRINGS, ATTENDER_NUMBER, STORED_POSITIONS))
    filled_extents = jnp.where(draw_filled_extents[0] < 3.0 / STORED_POSITIONS, jnp.log(0.5 + 0.3 * draw_filled_extents[1]), 0.0)
    return jnp.cumsum(decoding_logarithmic_decays + filled_extents, axis=-1).astype(jnp.float32)


def draw_keys_cache(key, part):
    split_prng_material = jax.random.split(jax.random.fold_in(key, 11), 1)
    base = jnp.clip(jax.random.normal(split_prng_material[0], (BATCH_STRINGS, STORED_POSITIONS, QW), jnp.float32), -6.0, 6.0)
    return base.astype(jnp.bfloat16)


def with_spikes(array, key, source, target, parts, factor):
    owner, partner = [(jnp.arange(array.shape[dim]) // (array.shape[dim] // parts)).reshape([-1 if axis == dim else 1 for axis in range(array.ndim)]) for dim in (source, target)]
    chosen = jax.random.permutation(key, parts)[partner]
    strong = (owner == chosen) | (owner == (partner + parts // 2) % parts)
    return jnp.where(strong, factor * array, array)


def level_of(rng, shape, pieces, least, top_value):
    level, own = 1.0, jax.random.fold_in(rng, 6)
    for position, parts in pieces:
        draws = jnp.exp(jax.random.uniform(jax.random.fold_in(own, position), (parts,), jnp.float32, least / len(pieces), top_value / len(pieces)))
        level = level * jnp.repeat(draws, shape[position] // parts).reshape([-1 if axis == position else 1 for axis in range(len(shape))])
    return level


def profile(number_of, total, most, slope):
    weights = [(1 << 20) // math.isqrt(grade ** slope) + 1 for grade in range(2, number_of + 1)]
    rest, counts = total - most - (number_of - 1), [1] * (number_of - 1)
    while rest > 0:
        candidates = [i for i in range(number_of - 1) if counts[i] < most]
        mass, left = sum([weights[i] for i in candidates]), rest
        for i in candidates:
            more = min(most - counts[i], max(1, left * weights[i] // mass), rest)
            counts[i] = counts[i] + more
            rest = rest - more
    return np.array([most] + counts)


def ragged_sizes(stream_key, number_of, total, bound, lean):
    if number_of == 2:
        one = jax.random.randint(stream_key, (), max(1, total - bound), min(bound, total - 1) + 1)
        return jnp.stack([one, total - one])
    sizes = jnp.asarray(profile(number_of, total, bound, lean), jnp.int32)
    couples = (number_of - 1) // 2
    giver, sink = sizes[1:1 + 2 * couples:2], sizes[2:2 + 2 * couples:2]
    slack = jnp.minimum(giver - 1, bound - sink)
    moved = jax.random.randint(jax.random.fold_in(stream_key, 1), (couples,), 0, 1 << 20) % (slack + 1)
    sizes = sizes.at[1:1 + 2 * couples:2].set(giver - moved).at[2:2 + 2 * couples:2].set(sink + moved)
    return sizes[jax.random.permutation(jax.random.fold_in(stream_key, 2), number_of)]


def normal_values(own_key, shape, width, most, shards=(), kind=jnp.bfloat16):
    result = width * jax.random.normal(own_key, shape, jnp.float32)
    if shards:
        result = result * level_of(own_key, shape, shards, -0.22, 0.18)
    return jnp.clip(result, -most, most).astype(kind)


def heavy_noise(rng, extent, width, reach, cuts, heavy, kind=jnp.bfloat16):
    drawn = width * jax.random.normal(rng, extent, jnp.float32)
    if cuts:
        drawn = drawn * level_of(rng, extent, cuts, -0.22, 0.18)
    return jnp.clip(with_spikes(drawn, jax.random.fold_in(rng, 3), *heavy), -reach, reach).astype(kind)


def setup_inputs(seed: int = 0) -> dict:
    streams_of = jax.random.split(jax.random.key(seed), 16)
    return {
        "tokens": normal_values(streams_of[0], (BATCH_STRINGS, D), 1.0, 6.0, ((1, 32),)),
        "gain_attn": jnp.clip(1.0 + 0.18 * jax.random.normal(streams_of[1], (D,), jnp.float32), 0.099609375, 1.8984375).astype(jnp.bfloat16),
        "w_query": normal_values(streams_of[2], (D, QW), D ** -0.5, 0.09375, ((0, 8), (1, 4))),
        "w_key": normal_values(streams_of[3], (D, QW), D ** -0.5, 0.09375, ((0, 8), (1, 4))),
        "w_value": normal_values(streams_of[4], (D, QW), D ** -0.5, 0.09375, ((0, 8), (1, 4))),
        "w_forget": normal_values(streams_of[5], (D, ATTENDER_NUMBER), D ** -0.5, 0.09375),
        "forget_bias": jnp.clip(jax.random.uniform(streams_of[6], (ATTENDER_NUMBER,), jnp.float32, -2.0, 2.0), -2.0, 2.0),
        "keys_cache": draw_keys_cache(jax.random.fold_in(streams_of[15], 71), 0),
        "values_cache": normal_values(streams_of[8], (BATCH_STRINGS, STORED_POSITIONS, QW), 1.0, 6.0, ((1, 8), (2, 4))),
        "gates_cache": draw_gates_cache(jax.random.fold_in(streams_of[15], 71), 0),
        "lengths": ragged_sizes(streams_of[10], BATCH_STRINGS, BATCH_STRINGS * STORED_POSITIONS // 2, STORED_POSITIONS, 2).astype(jnp.int32),
        "w_out": heavy_noise(streams_of[11], (QW, D), QW ** -0.5, 0.1875, ((0, 4), (1, 8)), (0, 1, 8, 2.0)),
        "gain_mixer": jnp.clip(1.0 + 0.18 * jax.random.normal(streams_of[12], (D,), jnp.float32), 0.099609375, 1.8984375).astype(jnp.bfloat16),
        "w_up": normal_values(streams_of[13], (D, FF), D ** -0.5, 0.09375, ((0, 8), (1, 4))),
        "w_down": heavy_noise(streams_of[14], (FF, D), FF ** -0.5, 0.0625, ((0, 4), (1, 8)), (0, 1, 8, 2.0)),
    }


norm_eps = 1e-06

def attend_one(items):
    query, keys, values, gates, length, forget_log, new_key, new_value = items
    heads = gates.shape[0]
    query_f = query.reshape(heads, -1).astype(jnp.float32)
    scale = query_f.shape[-1] ** (-0.5)
    keys_f = keys.reshape(keys.shape[0], heads, -1).astype(jnp.float32)
    values_f = values.reshape(values.shape[0], heads, -1).astype(jnp.float32)
    scores = jnp.einsum('hd,lhd->hl', query_f, keys_f) * scale
    last_gate = lax.dynamic_slice_in_dim(gates, (length - 1).astype(jnp.int32), 1, 1)[:, 0]
    logits = scores + (last_gate + forget_log)[:, None] - gates
    valid = jnp.arange(gates.shape[1], dtype=jnp.int32) < length
    logits = jnp.where(valid[None, :], logits, -jnp.inf)
    own = lax.optimization_barrier(jnp.sum(query_f * new_key.reshape(heads, -1).astype(jnp.float32), axis=-1)) * scale
    top = jnp.maximum(lax.optimization_barrier(jnp.max(logits, axis=-1)), own)
    weights = jnp.exp(logits - top[:, None])
    own_weight = jnp.exp(own - top)
    total = lax.optimization_barrier(jnp.sum(weights, axis=-1)) + own_weight
    rounded = weights.astype(jnp.bfloat16).astype(jnp.float32)
    summed = jnp.einsum('hl,lhd->hd', rounded, values_f)
    summed = summed + own_weight[:, None] * new_value.reshape(heads, -1).astype(jnp.float32)
    return (summed / total[:, None]).reshape(-1).astype(jnp.bfloat16)

def reference(tokens, gain_attn, w_query, w_key, w_value, w_forget, forget_bias, keys_cache, values_cache, gates_cache, lengths, w_out, gain_mixer, w_up, w_down):
    tokens_f = tokens.astype(jnp.float32)
    attn_scale = lax.rsqrt(lax.optimization_barrier(jnp.mean(tokens_f * tokens_f, axis=-1, keepdims=True)) + norm_eps)
    scaled_in = (tokens_f * gain_attn.astype(jnp.float32)).astype(jnp.bfloat16)
    query = (attn_scale * jnp.dot(scaled_in, w_query, preferred_element_type=jnp.float32)).astype(jnp.bfloat16)
    new_key = (attn_scale * jnp.dot(scaled_in, w_key, preferred_element_type=jnp.float32)).astype(jnp.bfloat16)
    new_value = (attn_scale * jnp.dot(scaled_in, w_value, preferred_element_type=jnp.float32)).astype(jnp.bfloat16)
    forget_log = jax.nn.log_sigmoid(attn_scale * jnp.dot(scaled_in, w_forget, preferred_element_type=jnp.float32) + forget_bias)
    mixed = lax.map(attend_one, (query, keys_cache, values_cache, gates_cache, lengths.astype(jnp.int32), forget_log, new_key, new_value))
    seqs = tokens.shape[0]
    group_width = mixed.shape[1] // N_TP
    mixed_groups = mixed.reshape(seqs, N_TP, group_width).astype(jnp.float32)
    out_groups = w_out.reshape(N_TP, group_width, -1).astype(jnp.float32)
    head_parts = jnp.einsum('bgk,gkd->gbd', mixed_groups, out_groups).astype(jnp.bfloat16)
    head_parts = lax.optimization_barrier(head_parts).astype(jnp.float32)
    residual = (tokens_f + lax.optimization_barrier(jnp.sum(head_parts, axis=0))).astype(jnp.bfloat16)
    residual_f = residual.astype(jnp.float32)
    mixer_scale = lax.rsqrt(lax.optimization_barrier(jnp.mean(residual_f * residual_f, axis=-1, keepdims=True)) + norm_eps)
    scaled_mid = (residual_f * gain_mixer.astype(jnp.float32)).astype(jnp.bfloat16)
    upward = jax.nn.relu(mixer_scale * jnp.dot(scaled_mid, w_up, preferred_element_type=jnp.float32))
    hidden = (upward * upward).astype(jnp.bfloat16)
    down = jnp.dot(hidden, w_down, preferred_element_type=jnp.float32)
    return (residual_f + down).astype(jnp.bfloat16)
```

```python
import functools

import jax
import jax.numpy as jnp
from jax import lax
from jax.experimental import pallas as pl
from jax.experimental.pallas import tpu as pltpu
from jax.sharding import PartitionSpec as P

norm_eps = 1e-06


def combined_all(value, axis, join):
    pieces = jax.tree.map(lambda part: lax.all_gather(part, axis), value)
    head = jax.tree.map(lambda part: part[0], pieces)
    tail = jax.tree.map(lambda part: part[1:], pieces)
    total, _ = lax.scan(lambda total, section: (join(total, section), None), head, tail)
    return total


def combine_parts(earlier, later):
    top = jnp.maximum(earlier[0], later[0])
    early_factor = jnp.exp(earlier[0] - top)
    late_factor = jnp.exp(later[0] - top)
    totals = earlier[1] * early_factor + later[1] * late_factor
    summed = earlier[2] * early_factor[..., None] + later[2] * late_factor[..., None]
    return (top, totals, summed, earlier[3] + later[3])


def channel_mix(residual, gain_mixer, w_up, w_down, kv_index):
    width = gain_mixer.shape[0]
    block_start = kv_index * w_up.shape[0]
    piece = lax.all_gather(residual, "tp", axis=1, tiled=True)
    piece_f = piece.astype(jnp.float32)
    gain_part = lax.dynamic_slice_in_dim(gain_mixer, block_start, piece.shape[1], 0).astype(
        jnp.float32
    )
    scaled = (piece_f * gain_part).astype(jnp.bfloat16)
    upward = jnp.dot(scaled, w_up, preferred_element_type=jnp.float32)
    upward, squares = (upward, jnp.sum(piece_f * piece_f, axis=-1))
    up_total, square_total = lax.psum((upward, squares), "kv")
    mixer_scale = lax.rsqrt(square_total / width + norm_eps)
    active = jax.nn.relu(mixer_scale[:, None] * up_total)
    hidden = (active * active).astype(jnp.bfloat16)
    down = jnp.dot(hidden, w_down, preferred_element_type=jnp.float32)
    return lax.psum_scatter(down, "tp", scatter_dimension=1, tiled=True)


def shards(
    tokens,
    gain_attn,
    w_query,
    w_key,
    w_value,
    w_forget,
    forget_bias,
    keys_cache,
    values_cache,
    gates_cache,
    lengths,
    w_out,
    gain_mixer,
    w_up,
    w_down,
):
    kv_index = lax.axis_index("kv")
    tp_index = lax.axis_index("tp")
    row_block = w_query.shape[0]
    heads_here = gates_cache.shape[1]
    width = gain_attn.shape[0]
    row_start = kv_index * row_block
    head_start = tp_index * heads_here
    block_raw = lax.all_gather(tokens, "tp", axis=1, tiled=True)
    block_f = block_raw.astype(jnp.float32)
    gain_block = lax.dynamic_slice_in_dim(gain_attn, row_start, row_block, 0).astype(jnp.float32)
    block = (block_f * gain_block).astype(jnp.bfloat16)
    forget_block = lax.dynamic_slice(w_forget, (row_start, head_start), (row_block, heads_here))
    part_query = jnp.dot(block, w_query, preferred_element_type=jnp.float32)
    part_key = jnp.dot(block, w_key, preferred_element_type=jnp.float32)
    part_value = jnp.dot(block, w_value, preferred_element_type=jnp.float32)
    part_gate = jnp.dot(block, forget_block, preferred_element_type=jnp.float32)
    part_squares = jnp.sum(block_f * block_f, axis=-1)
    sum_query, sum_key, sum_value, sum_gate, squares = lax.psum(
        (part_query, part_key, part_value, part_gate, part_squares), "kv"
    )
    attn_scale = lax.rsqrt(squares / width + norm_eps)[:, None]
    gate_logit = attn_scale * sum_gate
    query = (attn_scale * sum_query).astype(jnp.bfloat16)
    new_key = (attn_scale * sum_key).astype(jnp.bfloat16)
    new_value = (attn_scale * sum_value).astype(jnp.bfloat16)
    bias_here = lax.dynamic_slice_in_dim(forget_bias, head_start, heads_here, 0)
    forget_log = jax.nn.log_sigmoid(gate_logit + bias_here)
    seqs = tokens.shape[0]
    positions_here = keys_cache.shape[1]
    query_heads = query.reshape(seqs, heads_here, -1)
    head_size = query_heads.shape[-1]
    keys_heads = keys_cache.reshape(seqs, positions_here, heads_here, head_size)
    values_heads = values_cache.reshape(seqs, positions_here, heads_here, head_size)
    scores = jnp.einsum(
        "bhd,bphd->bhp", query_heads, keys_heads, preferred_element_type=jnp.float32
    )
    logits = scores * head_size ** (-0.5) - gates_cache
    positions = kv_index * positions_here + jnp.arange(positions_here, dtype=jnp.int32)
    valid = (positions[None, :] < lengths[:, None])[:, None, :]
    local_top = jnp.max(jnp.where(valid, logits, -1e30), axis=-1)
    weights = jnp.where(valid, jnp.exp(logits - local_top[..., None]), 0.0)
    local_total = jnp.sum(weights, axis=-1)
    local_sum = jnp.einsum(
        "bhp,bphd->bhd",
        weights.astype(jnp.bfloat16),
        values_heads,
        preferred_element_type=jnp.float32,
    )
    at_last = (positions[None, :] == lengths[:, None] - 1)[:, None, :]
    last_local = jnp.sum(jnp.where(at_last, gates_cache, 0.0), axis=-1)
    top, totals, summed, last_gate = combined_all(
        (local_top, local_total, local_sum, last_local), "kv", combine_parts
    )
    top = top + last_gate + forget_log
    own = jnp.sum(
        query_heads.astype(jnp.float32) * new_key.reshape(seqs, heads_here, -1).astype(jnp.float32),
        axis=-1,
    ) * head_size ** (-0.5)
    overall = jnp.maximum(top, own)
    cache_factor = jnp.exp(top - overall)
    own_weight = jnp.exp(own - overall)
    denominator = totals * cache_factor + own_weight
    numerator = summed * cache_factor[..., None] + own_weight[..., None] * new_value.reshape(
        seqs, heads_here, -1
    ).astype(jnp.float32)
    mixed = (numerator / denominator[..., None]).astype(jnp.bfloat16).reshape(seqs, -1)
    partial_value = jnp.dot(mixed, w_out, preferred_element_type=jnp.float32).astype(jnp.bfloat16)
    attended = lax.psum_scatter(partial_value, "tp", scatter_dimension=1, tiled=True).astype(
        jnp.float32
    )
    residual = (tokens.astype(jnp.float32) + attended).astype(jnp.bfloat16)
    mixer = channel_mix(residual, gain_mixer, w_up, w_down, kv_index)
    return (residual.astype(jnp.float32) + mixer).astype(jnp.bfloat16)


f32, bf16 = jnp.float32, jnp.bfloat16
LANES = 128


def split_squares(values):
    total = jnp.sum(values * values, axis=-1, keepdims=True)
    high = total.astype(bf16).astype(f32)
    lane = lax.broadcasted_iota(jnp.int32, (values.shape[0], LANES), 1)
    return jnp.where(lane == 0, high, jnp.where(lane == 1, total - high, 0.0))


def joined_squares(block):
    return jnp.sum(block, axis=-1, keepdims=True)


def fused(
    n_kv,
    n_tp,
    tokens,
    gain_attn,
    forget_bias,
    lengths,
    gain_mixer,
    w_query,
    w_key,
    w_value,
    w_forget,
    keys_cache,
    values_cache,
    gates_cache,
    w_out,
    w_up,
    w_down,
    out,
    wq,
    wk,
    wv,
    wf,
    keys,
    values,
    gates,
    wo,
    wu,
    wd,
    tok_all,
    q_send,
    q_all,
    p_send,
    p_all,
    a_send,
    a_all,
    m_send,
    m_all,
    o_send,
    o_all,
    u_send,
    u_all,
    h_send,
    h_all,
    f_send,
    f_all,
    query,
    mix,
    res,
    load_sem,
    kv_out,
    kv_in,
    tp_out,
    tp_in,
):
    kv, tp = lax.axis_index("kv"), lax.axis_index("tp")
    seqs, piece = tokens.shape
    rows, cols = wq.shape
    positions = keys.shape[1]
    heads = gates.shape[1]
    all_heads = wf.shape[1]
    size = cols // heads
    mine = seqs // n_kv
    width = gain_attn.shape[1]
    unit = wu.shape[1] // n_kv

    row_at = pl.multiple_of(kv * rows, rows)
    sources = [
        (w_query, wq),
        (w_key, wk),
        (w_value, wv),
        (w_forget.at[pl.ds(row_at, rows), :], wf),
        (keys_cache, keys),
        (gates_cache, gates),
        (values_cache, values),
        (w_out, wo),
        (w_up, wu),
        (w_down, wd),
    ]
    loads = [pltpu.make_async_copy(a, b, load_sem.at[i]) for i, (a, b) in enumerate(sources)]
    for load in loads:
        load.start()
    ld_q, ld_k, ld_v, ld_f, ld_keys, ld_gates, ld_values, ld_o, ld_u, ld_d = loads

    barrier = pltpu.get_barrier_semaphore()
    for j in range(1, n_kv):
        pl.semaphore_signal(
            barrier,
            inc=1,
            device_id=(lax.rem(kv + j, n_kv), tp),
            device_id_type=pl.DeviceIdType.MESH,
        )
    for j in range(1, n_tp):
        pl.semaphore_signal(
            barrier,
            inc=1,
            device_id=(kv, lax.rem(tp + j, n_tp)),
            device_id_type=pl.DeviceIdType.MESH,
        )
    pl.semaphore_wait(barrier, n_kv + n_tp - 2)

    def over_kv(phase, j, source, landing):
        peer = lax.rem(kv + j, n_kv)
        return pltpu.make_async_remote_copy(
            src_ref=source(peer),
            dst_ref=landing.at[kv],
            send_sem=kv_out.at[phase, j],
            recv_sem=kv_in.at[phase, kv],
            device_id=(peer, tp),
            device_id_type=pl.DeviceIdType.MESH,
        )

    def from_kv(phase, j, source, landing):
        peer = lax.rem(kv + n_kv - j, n_kv)
        pltpu.make_async_remote_copy(
            src_ref=source(peer),
            dst_ref=landing.at[peer],
            send_sem=kv_out.at[phase, j],
            recv_sem=kv_in.at[phase, peer],
            device_id=(peer, tp),
            device_id_type=pl.DeviceIdType.MESH,
        ).wait_recv()
        return peer

    def over_tp(phase, j, source, landing):
        peer = lax.rem(tp + j, n_tp)
        return pltpu.make_async_remote_copy(
            src_ref=source(peer),
            dst_ref=landing.at[tp],
            send_sem=tp_out.at[phase, j],
            recv_sem=tp_in.at[phase, tp],
            device_id=(kv, peer),
            device_id_type=pl.DeviceIdType.MESH,
        )

    def from_tp(phase, j, source, landing):
        peer = lax.rem(tp + n_tp - j, n_tp)
        pltpu.make_async_remote_copy(
            src_ref=source(peer),
            dst_ref=landing.at[peer],
            send_sem=tp_out.at[phase, j],
            recv_sem=tp_in.at[phase, peer],
            device_id=(kv, peer),
            device_id_type=pl.DeviceIdType.MESH,
        ).wait_recv()
        return peer

    pending = []

    def send_kv(phase, j, source, landing):
        copy = over_kv(phase, j, source, landing)
        copy.start()
        pending.append(copy)

    def send_tp(phase, j, source, landing):
        copy = over_tp(phase, j, source, landing)
        copy.start()
        pending.append(copy)

    for j in range(1, n_tp):
        send_tp(0, j, lambda peer: tokens, tok_all)
    tok_all[tp] = tokens[...]
    gain_a = gain_attn[:, pl.ds(row_at, rows)].astype(f32)
    gain_m = gain_mixer[:, pl.ds(row_at, rows)].astype(f32)
    for j in range(1, n_tp):
        from_tp(0, j, lambda peer: tokens, tok_all)
    tok = jnp.concatenate([tok_all[t] for t in range(n_tp)], axis=1).astype(f32)
    scaled = (tok * gain_a).astype(bf16)

    ld_q.wait()
    squares = split_squares(tok)
    q_send[:, :cols] = jnp.dot(scaled, wq[...], preferred_element_type=f32).astype(bf16)
    q_send[:, cols:] = squares.astype(bf16)
    for j in range(1, n_kv):
        send_kv(0, j, lambda peer: q_send, q_all)
    q_all[kv] = q_send[...]

    ld_k.wait()
    ld_v.wait()
    ld_f.wait()
    part_key = jnp.dot(scaled, wk[...], preferred_element_type=f32)
    part_value = jnp.dot(scaled, wv[...], preferred_element_type=f32)
    part_gate = jnp.dot(scaled, wf[...], preferred_element_type=f32)
    for o in range(n_kv):
        at = slice(o * mine, (o + 1) * mine)
        p_send[o, :, :cols] = part_key[at]
        p_send[o, :, cols : 2 * cols] = part_value[at]
        p_send[o, :, 2 * cols : 2 * cols + all_heads] = part_gate[at]
        p_send[o, :, 2 * cols + all_heads :] = jnp.zeros((mine, LANES - all_heads), f32)
    for j in range(1, n_kv):
        send_kv(1, j, lambda peer: p_send.at[peer], p_all)
    p_all[kv] = p_send[kv]

    for j in range(1, n_kv):
        from_kv(0, j, lambda peer: q_send, q_all)
    q_total = q_all[0].astype(f32)
    for o in range(1, n_kv):
        q_total = q_total + q_all[o].astype(f32)
    attn_scale = lax.rsqrt(joined_squares(q_total[:, cols:]) / width + norm_eps)
    query[:, :cols] = (attn_scale * q_total[:, :cols]).astype(bf16).astype(f32)
    query[:, cols:] = jnp.broadcast_to(attn_scale, (seqs, LANES))

    ld_keys.wait()
    ld_gates.wait()
    ld_values.wait()
    head_row = lax.broadcasted_iota(jnp.int32, (heads, cols), 0)
    own_block = head_row == lax.broadcasted_iota(jnp.int32, (heads, cols), 1) // size
    place = kv * positions + lax.broadcasted_iota(jnp.int32, (heads, positions), 1)
    stat_row = lax.broadcasted_iota(jnp.int32, (heads, LANES), 0)
    stat_lane = lax.broadcasted_iota(jnp.int32, (heads, LANES), 1)

    def attend(owner):
        for r in range(mine):
            b = owner * mine + r
            spread = jnp.where(own_block, query[pl.ds(b, 1), :cols], 0.0).astype(bf16)
            scores = lax.dot_general(
                spread, keys[b], (((1,), (1,)), ((), ())), preferred_element_type=f32
            )
            gate = gates[b]
            length = lengths[b]
            valid = place < length
            logits = scores * size ** (-0.5) - gate
            top = jnp.max(jnp.where(valid, logits, -1e30), axis=-1, keepdims=True)
            weights = jnp.where(valid, jnp.exp(logits - top), 0.0)
            total = jnp.sum(weights, axis=-1, keepdims=True)
            last = jnp.sum(jnp.where(place == length - 1, gate, 0.0), axis=-1, keepdims=True)
            summed = jnp.dot(weights.astype(bf16), values[b], preferred_element_type=f32)
            a_send[owner, r : r + 1, :cols] = jnp.sum(
                jnp.where(own_block, summed, 0.0), axis=0, keepdims=True
            )
            stats = jnp.where(
                stat_lane == stat_row,
                top,
                jnp.where(
                    stat_lane == stat_row + heads,
                    total,
                    jnp.where(stat_lane == stat_row + 2 * heads, last, 0.0),
                ),
            )
            a_send[owner, r : r + 1, cols:] = jnp.sum(stats, axis=0, keepdims=True)

    def attend_for(j, carry):
        attend(lax.rem(kv + j, n_kv))
        over_kv(2, j, lambda peer: a_send.at[peer], a_all).start()
        return carry

    lax.fori_loop(1, n_kv, attend_for, 0)
    attend(kv)
    a_all[kv] = a_send[kv]

    for j in range(1, n_kv):
        from_kv(1, j, lambda peer: p_send.at[peer], p_all)
    p_total = p_all[0]
    for o in range(1, n_kv):
        p_total = p_total + p_all[o]
    own_rows = [query[pl.ds(kv * mine + r, 1), :] for r in range(mine)]
    own_query = jnp.concatenate(own_rows, axis=0)
    own_scale = own_query[:, cols : cols + 1]
    own_query = own_query[:, :cols]
    new_key = (own_scale * p_total[:, :cols]).astype(bf16).astype(f32)
    new_value = (own_scale * p_total[:, cols : 2 * cols]).astype(bf16).astype(f32)
    gate_logit = own_scale * p_total[:, 2 * cols : 2 * cols + all_heads] + forget_bias[...]
    forget_log = jnp.minimum(gate_logit, 0.0) - jnp.log1p(jnp.exp(-jnp.abs(gate_logit)))
    col_head = lax.broadcasted_iota(jnp.int32, (mine, cols), 1) // size
    forget_wide = jnp.zeros((mine, cols), f32)
    for h in range(all_heads):
        forget_wide = jnp.where(col_head + tp * heads == h, forget_log[:, h : h + 1], forget_wide)
    product = own_query * new_key
    own = jnp.zeros((mine, cols), f32)
    for h in range(heads):
        inside = col_head == h
        own = jnp.where(
            inside, jnp.sum(jnp.where(inside, product, 0.0), axis=-1, keepdims=True), own
        )
    own = own * size ** (-0.5)

    for j in range(1, n_kv):
        from_kv(2, j, lambda peer: a_send.at[peer], a_all)

    def wide(part, first):
        result = jnp.zeros((mine, cols), f32)
        for h in range(heads):
            result = jnp.where(col_head == h, part[:, first + h : first + h + 1], result)
        return result

    tops = [wide(a_all[o, :, cols:], 0) for o in range(n_kv)]
    top = functools.reduce(jnp.maximum, tops)
    totals = jnp.zeros((mine, cols), f32)
    summed = jnp.zeros((mine, cols), f32)
    stat_sum = a_all[0, :, cols:]
    for o in range(1, n_kv):
        stat_sum = stat_sum + a_all[o, :, cols:]
    for o in range(n_kv):
        factor = jnp.exp(tops[o] - top)
        totals = totals + factor * wide(a_all[o, :, cols:], heads)
        summed = summed + factor * a_all[o, :, :cols]
    top = top + wide(stat_sum, 2 * heads) + forget_wide
    overall = jnp.maximum(top, own)
    cache_factor = jnp.exp(top - overall)
    own_weight = jnp.exp(own - overall)
    denominator = totals * cache_factor + own_weight
    numerator = summed * cache_factor + own_weight * new_value
    m_send[...] = (numerator / denominator).astype(bf16).astype(f32)
    for j in range(1, n_kv):
        send_kv(3, j, lambda peer: m_send, m_all)
    m_all[kv] = m_send[...]
    ld_o.wait()
    for j in range(1, n_kv):
        from_kv(3, j, lambda peer: m_send, m_all)
    for o in range(n_kv):
        mix[o * mine : (o + 1) * mine, :] = m_all[o]

    o_send[...] = jnp.dot(mix[...].astype(bf16), wo[...], preferred_element_type=f32).astype(bf16)
    for j in range(1, n_tp):
        send_tp(1, j, lambda peer: o_send, o_all)
    o_all[tp] = o_send[...]
    ld_u.wait()
    for j in range(1, n_tp):
        from_tp(1, j, lambda peer: o_send, o_all)
    attended = o_all[0].astype(f32)
    for t in range(1, n_tp):
        attended = attended + o_all[t].astype(f32)
    residual = (tok + attended).astype(bf16).astype(f32)
    for t in range(n_tp):
        res[t] = residual[:, t * piece : (t + 1) * piece]

    scaled_mid = (residual * gain_m).astype(bf16)
    squares_mid = split_squares(residual).astype(bf16)

    def up_piece(owner):
        at = pl.multiple_of(owner * unit, unit)
        u_send[owner, :, :unit] = jnp.dot(
            scaled_mid, wu[:, pl.ds(at, unit)], preferred_element_type=f32
        ).astype(bf16)
        u_send[owner, :, unit:] = squares_mid

    for j in range(1, n_kv):
        up_piece(lax.rem(kv + j, n_kv))
        send_kv(4, j, lambda peer: u_send.at[peer], u_all)
    up_piece(kv)
    u_all[kv] = u_send[kv]
    for j in range(1, n_kv):
        from_kv(4, j, lambda peer: u_send.at[peer], u_all)
    up_total = u_all[0].astype(f32)
    for o in range(1, n_kv):
        up_total = up_total + u_all[o].astype(f32)
    mixer_scale = lax.rsqrt(joined_squares(up_total[:, unit:]) / width + norm_eps)
    active = jnp.maximum(mixer_scale * up_total[:, :unit], 0.0)
    h_send[...] = (active * active).astype(bf16)
    for j in range(1, n_kv):
        send_kv(5, j, lambda peer: h_send, h_all)

    ld_d.wait()

    def down_piece(block, owner):
        at = pl.multiple_of(owner * unit, unit)
        return jnp.dot(block, wd[pl.ds(at, unit), :], preferred_element_type=f32)

    down = down_piece(h_send[...], kv)
    for j in range(1, n_kv):
        peer = from_kv(5, j, lambda peer: h_send, h_all)
        down = down + down_piece(h_all[peer], peer)
    for t in range(n_tp):
        f_send[t] = down[:, t * piece : (t + 1) * piece]
    for j in range(1, n_tp):
        send_tp(2, j, lambda peer: f_send.at[peer], f_all)
    f_all[tp] = f_send[tp]
    for j in range(1, n_tp):
        from_tp(2, j, lambda peer: f_send.at[peer], f_all)
    mixer = f_all[0]
    for t in range(1, n_tp):
        mixer = mixer + f_all[t]
    out[...] = (res[tp] + mixer).astype(bf16)

    for copy in pending:
        copy.wait_send()
    for j in range(1, n_kv):
        over_kv(2, j, lambda peer: a_send.at[peer], a_all).wait_send()


def layer(n_kv, n_tp, *arrays):
    (
        tokens,
        gain_attn,
        w_query,
        w_key,
        w_value,
        w_forget,
        forget_bias,
        keys_cache,
        values_cache,
        gates_cache,
        lengths,
        w_out,
        gain_mixer,
        w_up,
        w_down,
    ) = arrays
    seqs, piece = tokens.shape
    rows, cols = w_query.shape
    heads = gates_cache.shape[1]
    all_heads = w_forget.shape[1]
    unit = w_up.shape[1] // n_kv
    fits = (
        piece % LANES == 0
        and cols % LANES == 0
        and unit % LANES == 0
        and seqs % n_kv == 0
        and 3 * heads <= LANES
        and all_heads < LANES
        and w_out.shape == (cols, rows)
        and n_kv > 1
        and n_tp > 1
    )
    if not fits:
        return shards(*arrays)
    mine = seqs // n_kv
    vmem = pl.BlockSpec(memory_space=pltpu.VMEM)
    smem = pl.BlockSpec(memory_space=pltpu.SMEM)
    anywhere = pl.BlockSpec(memory_space=pl.ANY)

    def like(x):
        return pltpu.VMEM(x.shape, x.dtype)

    return pl.pallas_call(
        functools.partial(fused, n_kv, n_tp),
        out_shape=jax.ShapeDtypeStruct((seqs, piece), bf16),
        in_specs=[vmem, vmem, vmem, smem, vmem] + [anywhere] * 10,
        out_specs=vmem,
        scratch_shapes=[
            like(w_query),
            like(w_key),
            like(w_value),
            pltpu.VMEM((rows, all_heads), bf16),
            like(keys_cache),
            like(values_cache),
            like(gates_cache),
            like(w_out),
            like(w_up),
            like(w_down),
            pltpu.VMEM((n_tp, seqs, piece), bf16),
            pltpu.VMEM((seqs, cols + LANES), bf16),
            pltpu.VMEM((n_kv, seqs, cols + LANES), bf16),
            pltpu.VMEM((n_kv, mine, 2 * cols + LANES), f32),
            pltpu.VMEM((n_kv, mine, 2 * cols + LANES), f32),
            pltpu.VMEM((n_kv, mine, cols + LANES), f32),
            pltpu.VMEM((n_kv, mine, cols + LANES), f32),
            pltpu.VMEM((mine, cols), f32),
            pltpu.VMEM((n_kv, mine, cols), f32),
            pltpu.VMEM((seqs, rows), bf16),
            pltpu.VMEM((n_tp, seqs, rows), bf16),
            pltpu.VMEM((n_kv, seqs, unit + LANES), bf16),
            pltpu.VMEM((n_kv, seqs, unit + LANES), bf16),
            pltpu.VMEM((seqs, unit), bf16),
            pltpu.VMEM((n_kv, seqs, unit), bf16),
            pltpu.VMEM((n_tp, seqs, piece), f32),
            pltpu.VMEM((n_tp, seqs, piece), f32),
            pltpu.VMEM((seqs, cols + LANES), f32),
            pltpu.VMEM((seqs, cols), f32),
            pltpu.VMEM((n_tp, seqs, piece), f32),
            pltpu.SemaphoreType.DMA((10,)),
            pltpu.SemaphoreType.DMA((6, n_kv)),
            pltpu.SemaphoreType.DMA((6, n_kv)),
            pltpu.SemaphoreType.DMA((3, n_tp)),
            pltpu.SemaphoreType.DMA((3, n_tp)),
        ],
        compiler_params=pltpu.CompilerParams(
            collective_id=0, has_side_effects=True, vmem_limit_bytes=60 * 1024 * 1024
        ),
    )(
        tokens,
        gain_attn.reshape(1, -1),
        forget_bias.reshape(1, -1),
        lengths,
        gain_mixer.reshape(1, -1),
        w_query,
        w_key,
        w_value,
        w_forget,
        keys_cache,
        values_cache,
        gates_cache,
        w_out,
        w_up,
        w_down,
    )


def solution(mesh):
    return jax.shard_map(
        functools.partial(layer, mesh.shape["kv"], mesh.shape["tp"]),
        mesh=mesh,
        in_specs=(
            P(None, ("kv", "tp")),
            P(),
            P("kv", "tp"),
            P("kv", "tp"),
            P("kv", "tp"),
            P(),
            P(),
            P(None, "kv", "tp"),
            P(None, "kv", "tp"),
            P(None, "tp", "kv"),
            P(),
            P("tp", "kv"),
            P(),
            P("kv", "tp"),
            P("tp", "kv"),
        ),
        out_specs=P(None, ("kv", "tp")),
        check_vma=False,
    )
```

```python
import functools

import jax
import jax.numpy as jnp
from jax import lax
from jax.experimental import pallas as pl
from jax.experimental.pallas import tpu as pltpu
from jax.sharding import PartitionSpec as P

norm_eps = 1e-06


def combined_all(value, axis, join):
    pieces = jax.tree.map(lambda part: lax.all_gather(part, axis), value)
    head = jax.tree.map(lambda part: part[0], pieces)
    tail = jax.tree.map(lambda part: part[1:], pieces)
    total, _ = lax.scan(lambda total, section: (join(total, section), None), head, tail)
    return total


def combine_parts(earlier, later):
    top = jnp.maximum(earlier[0], later[0])
    early_factor = jnp.exp(earlier[0] - top)
    late_factor = jnp.exp(later[0] - top)
    totals = earlier[1] * early_factor + later[1] * late_factor
    summed = earlier[2] * early_factor[..., None] + later[2] * late_factor[..., None]
    return (top, totals, summed, earlier[3] + later[3])


def channel_mix(residual, gain_mixer, w_up, w_down, kv_index):
    width = gain_mixer.shape[0]
    block_start = kv_index * w_up.shape[0]
    piece = lax.all_gather(residual, "tp", axis=1, tiled=True)
    piece_f = piece.astype(jnp.float32)
    gain_part = lax.dynamic_slice_in_dim(gain_mixer, block_start, piece.shape[1], 0).astype(
        jnp.float32
    )
    scaled = (piece_f * gain_part).astype(jnp.bfloat16)
    upward = jnp.dot(scaled, w_up, preferred_element_type=jnp.float32)
    upward, squares = (upward, jnp.sum(piece_f * piece_f, axis=-1))
    up_total, square_total = lax.psum((upward, squares), "kv")
    mixer_scale = lax.rsqrt(square_total / width + norm_eps)
    active = jax.nn.relu(mixer_scale[:, None] * up_total)
    hidden = (active * active).astype(jnp.bfloat16)
    down = jnp.dot(hidden, w_down, preferred_element_type=jnp.float32)
    return lax.psum_scatter(down, "tp", scatter_dimension=1, tiled=True)


def shards(
    tokens,
    gain_attn,
    w_query,
    w_key,
    w_value,
    w_forget,
    forget_bias,
    keys_cache,
    values_cache,
    gates_cache,
    lengths,
    w_out,
    gain_mixer,
    w_up,
    w_down,
):
    kv_index = lax.axis_index("kv")
    tp_index = lax.axis_index("tp")
    row_block = w_query.shape[0]
    heads_here = gates_cache.shape[1]
    width = gain_attn.shape[0]
    row_start = kv_index * row_block
    head_start = tp_index * heads_here
    block_raw = lax.all_gather(tokens, "tp", axis=1, tiled=True)
    block_f = block_raw.astype(jnp.float32)
    gain_block = lax.dynamic_slice_in_dim(gain_attn, row_start, row_block, 0).astype(jnp.float32)
    block = (block_f * gain_block).astype(jnp.bfloat16)
    forget_block = lax.dynamic_slice(w_forget, (row_start, head_start), (row_block, heads_here))
    part_query = jnp.dot(block, w_query, preferred_element_type=jnp.float32)
    part_key = jnp.dot(block, w_key, preferred_element_type=jnp.float32)
    part_value = jnp.dot(block, w_value, preferred_element_type=jnp.float32)
    part_gate = jnp.dot(block, forget_block, preferred_element_type=jnp.float32)
    part_squares = jnp.sum(block_f * block_f, axis=-1)
    sum_query, sum_key, sum_value, sum_gate, squares = lax.psum(
        (part_query, part_key, part_value, part_gate, part_squares), "kv"
    )
    attn_scale = lax.rsqrt(squares / width + norm_eps)[:, None]
    gate_logit = attn_scale * sum_gate
    query = (attn_scale * sum_query).astype(jnp.bfloat16)
    new_key = (attn_scale * sum_key).astype(jnp.bfloat16)
    new_value = (attn_scale * sum_value).astype(jnp.bfloat16)
    bias_here = lax.dynamic_slice_in_dim(forget_bias, head_start, heads_here, 0)
    forget_log = jax.nn.log_sigmoid(gate_logit + bias_here)
    seqs = tokens.shape[0]
    positions_here = keys_cache.shape[1]
    query_heads = query.reshape(seqs, heads_here, -1)
    head_size = query_heads.shape[-1]
    keys_heads = keys_cache.reshape(seqs, positions_here, heads_here, head_size)
    values_heads = values_cache.reshape(seqs, positions_here, heads_here, head_size)
    scores = jnp.einsum(
        "bhd,bphd->bhp", query_heads, keys_heads, preferred_element_type=jnp.float32
    )
    logits = scores * head_size ** (-0.5) - gates_cache
    positions = kv_index * positions_here + jnp.arange(positions_here, dtype=jnp.int32)
    valid = (positions[None, :] < lengths[:, None])[:, None, :]
    local_top = jnp.max(jnp.where(valid, logits, -1e30), axis=-1)
    weights = jnp.where(valid, jnp.exp(logits - local_top[..., None]), 0.0)
    local_total = jnp.sum(weights, axis=-1)
    local_sum = jnp.einsum(
        "bhp,bphd->bhd",
        weights.astype(jnp.bfloat16),
        values_heads,
        preferred_element_type=jnp.float32,
    )
    at_last = (positions[None, :] == lengths[:, None] - 1)[:, None, :]
    last_local = jnp.sum(jnp.where(at_last, gates_cache, 0.0), axis=-1)
    top, totals, summed, last_gate = combined_all(
        (local_top, local_total, local_sum, last_local), "kv", combine_parts
    )
    top = top + last_gate + forget_log
    own = jnp.sum(
        query_heads.astype(jnp.float32) * new_key.reshape(seqs, heads_here, -1).astype(jnp.float32),
        axis=-1,
    ) * head_size ** (-0.5)
    overall = jnp.maximum(top, own)
    cache_factor = jnp.exp(top - overall)
    own_weight = jnp.exp(own - overall)
    denominator = totals * cache_factor + own_weight
    numerator = summed * cache_factor[..., None] + own_weight[..., None] * new_value.reshape(
        seqs, heads_here, -1
    ).astype(jnp.float32)
    mixed = (numerator / denominator[..., None]).astype(jnp.bfloat16).reshape(seqs, -1)
    partial_value = jnp.dot(mixed, w_out, preferred_element_type=jnp.float32).astype(jnp.bfloat16)
    attended = lax.psum_scatter(partial_value, "tp", scatter_dimension=1, tiled=True).astype(
        jnp.float32
    )
    residual = (tokens.astype(jnp.float32) + attended).astype(jnp.bfloat16)
    mixer = channel_mix(residual, gain_mixer, w_up, w_down, kv_index)
    return (residual.astype(jnp.float32) + mixer).astype(jnp.bfloat16)


f32, bf16 = jnp.float32, jnp.bfloat16
LANES = 128


def to_row(column):
    shape = (column.shape[0], LANES)
    same = lax.broadcasted_iota(jnp.int32, shape, 0) == lax.broadcasted_iota(jnp.int32, shape, 1)
    return jnp.sum(jnp.where(same, column, 0.0), axis=0, keepdims=True)


def to_column(row, count):
    shape = (count, LANES)
    same = lax.broadcasted_iota(jnp.int32, shape, 0) == lax.broadcasted_iota(jnp.int32, shape, 1)
    return jnp.sum(jnp.where(same, row, 0.0), axis=-1, keepdims=True)


def fused(
    n_kv,
    n_tp,
    tokens,
    gain_attn,
    forget_bias,
    lengths,
    gain_mixer,
    w_query,
    w_key,
    w_value,
    w_forget,
    keys_cache,
    values_cache,
    gates_cache,
    w_out,
    w_up,
    w_down,
    out,
    wq,
    wk,
    wv,
    wf,
    keys,
    values,
    gates,
    wo,
    wu,
    wd,
    tok_all,
    q_send,
    q_all,
    p_send,
    p_all,
    a_send,
    a_all,
    m_send,
    m_all,
    o_send,
    o_all,
    u_send,
    u_all,
    h_send,
    h_all,
    f_send,
    f_all,
    query,
    mix,
    res,
    s_send,
    s_all,
    load_sem,
    kv_out,
    kv_in,
    tp_out,
    tp_in,
):
    kv, tp = lax.axis_index("kv"), lax.axis_index("tp")
    seqs, piece = tokens.shape
    rows, cols = wq.shape
    positions = keys.shape[1]
    heads = gates.shape[1]
    all_heads = wf.shape[0]
    size = cols // heads
    mine = seqs // n_kv
    width = gain_attn.shape[0]
    unit = wu.shape[1] // n_kv

    row_at = pl.multiple_of(kv * rows, rows)
    sources = [
        (w_query, wq),
        (w_key, wk),
        (w_value, wv),
        (w_forget.at[:, pl.ds(row_at, rows)], wf),
        (keys_cache, keys),
        (gates_cache, gates),
        (values_cache, values),
        (w_out, wo),
        (w_up, wu),
        (w_down, wd),
    ]
    loads = [pltpu.make_async_copy(a, b, load_sem.at[i]) for i, (a, b) in enumerate(sources)]
    for load in loads:
        load.start()
    ld_q, ld_k, ld_v, ld_f, ld_keys, ld_gates, ld_values, ld_o, ld_u, ld_d = loads

    barrier = pltpu.get_barrier_semaphore()
    for j in range(1, n_kv):
        pl.semaphore_signal(
            barrier,
            inc=1,
            device_id=(lax.rem(kv + j, n_kv), tp),
            device_id_type=pl.DeviceIdType.MESH,
        )
    for j in range(1, n_tp):
        pl.semaphore_signal(
            barrier,
            inc=1,
            device_id=(kv, lax.rem(tp + j, n_tp)),
            device_id_type=pl.DeviceIdType.MESH,
        )
    pl.semaphore_wait(barrier, n_kv + n_tp - 2)

    turn = 2 * (kv // (n_kv // 2)) - 1

    def kv_peer(j):
        return lax.rem(kv + turn * j + n_kv, n_kv)

    def over_kv(phase, j, source, landing):
        peer = kv_peer(j)
        return pltpu.make_async_remote_copy(
            src_ref=source(peer),
            dst_ref=landing.at[kv],
            send_sem=kv_out.at[phase, j],
            recv_sem=kv_in.at[phase, kv],
            device_id=(peer, tp),
            device_id_type=pl.DeviceIdType.MESH,
        )

    def from_kv(phase, j, source, landing):
        peer = lax.rem(kv - turn * j + n_kv, n_kv)
        pltpu.make_async_remote_copy(
            src_ref=source(peer),
            dst_ref=landing.at[peer],
            send_sem=kv_out.at[phase, j],
            recv_sem=kv_in.at[phase, peer],
            device_id=(peer, tp),
            device_id_type=pl.DeviceIdType.MESH,
        ).wait_recv()
        return peer

    def over_tp(phase, j, source, landing):
        peer = lax.rem(tp + j, n_tp)
        return pltpu.make_async_remote_copy(
            src_ref=source(peer),
            dst_ref=landing.at[tp],
            send_sem=tp_out.at[phase, j],
            recv_sem=tp_in.at[phase, tp],
            device_id=(kv, peer),
            device_id_type=pl.DeviceIdType.MESH,
        )

    def from_tp(phase, j, source, landing):
        peer = lax.rem(tp + n_tp - j, n_tp)
        pltpu.make_async_remote_copy(
            src_ref=source(peer),
            dst_ref=landing.at[peer],
            send_sem=tp_out.at[phase, j],
            recv_sem=tp_in.at[phase, peer],
            device_id=(kv, peer),
            device_id_type=pl.DeviceIdType.MESH,
        ).wait_recv()
        return peer

    pending = []

    def send_kv(phase, j, source, landing):
        copy = over_kv(phase, j, source, landing)
        copy.start()
        pending.append(copy)

    def send_tp(phase, j, source, landing):
        copy = over_tp(phase, j, source, landing)
        copy.start()
        pending.append(copy)

    def share_squares(which, block):
        column = jnp.sum(block * block, axis=-1, keepdims=True)
        s_send[which] = to_row(column)
        for j in range(1, n_kv):
            send_kv(6 + which, j, lambda peer: s_send.at[which], s_all.at[which])
        s_all[which, kv] = s_send[which]

    def joined_squares(which):
        for j in range(1, n_kv):
            from_kv(6 + which, j, lambda peer: s_send.at[which], s_all.at[which])
        total = s_all[which, 0]
        for o in range(1, n_kv):
            total = total + s_all[which, o]
        return to_column(total, seqs)

    for j in range(1, n_tp):
        send_tp(0, j, lambda peer: tokens, tok_all)
    tok_all[tp] = tokens[...]
    gain_a = gain_attn[pl.ds(row_at, rows)].astype(f32).reshape(1, rows)
    gain_m = gain_mixer[pl.ds(row_at, rows)].astype(f32).reshape(1, rows)
    for j in range(1, n_tp):
        from_tp(0, j, lambda peer: tokens, tok_all)
    tok = jnp.concatenate([tok_all[t] for t in range(n_tp)], axis=1).astype(f32)
    scaled = (tok * gain_a).astype(bf16)

    share_squares(0, tok)

    ld_q.wait()
    q_send[...] = jnp.dot(scaled, wq[...], preferred_element_type=f32).astype(bf16)
    for j in range(1, n_kv):
        send_kv(0, j, lambda peer: q_send, q_all)
    q_all[kv] = q_send[...]

    ld_k.wait()
    ld_v.wait()
    ld_f.wait()
    part_key = jnp.dot(scaled, wk[...], preferred_element_type=f32)
    part_value = jnp.dot(scaled, wv[...], preferred_element_type=f32)
    part_gate = lax.dot_general(
        scaled, wf[...], (((1,), (1,)), ((), ())), preferred_element_type=f32
    )
    for o in range(n_kv):
        at = slice(o * mine, (o + 1) * mine)
        p_send[o, :, :cols] = part_key[at]
        p_send[o, :, cols : 2 * cols] = part_value[at]
        p_send[o, :, 2 * cols : 2 * cols + all_heads] = part_gate[at]
        p_send[o, :, 2 * cols + all_heads :] = jnp.zeros((mine, LANES - all_heads), f32)
    for j in range(1, n_kv):
        send_kv(1, j, lambda peer: p_send.at[peer], p_all)
    p_all[kv] = p_send[kv]

    for j in range(1, n_kv):
        from_kv(0, j, lambda peer: q_send, q_all)
    q_total = q_all[0].astype(f32)
    for o in range(1, n_kv):
        q_total = q_total + q_all[o].astype(f32)
    attn_scale = lax.rsqrt(joined_squares(0) / width + norm_eps)
    query[:, :cols] = (attn_scale * q_total).astype(bf16).astype(f32)
    query[:, cols:] = jnp.broadcast_to(attn_scale, (seqs, LANES))

    ld_keys.wait()
    ld_gates.wait()
    ld_values.wait()
    head_row = lax.broadcasted_iota(jnp.int32, (heads, cols), 0)
    own_block = head_row == lax.broadcasted_iota(jnp.int32, (heads, cols), 1) // size
    place = kv * positions + lax.broadcasted_iota(jnp.int32, (heads, positions), 1)
    stat_row = lax.broadcasted_iota(jnp.int32, (heads, LANES), 0)
    stat_lane = lax.broadcasted_iota(jnp.int32, (heads, LANES), 1)

    def attend(owner):
        for r in range(mine):
            b = owner * mine + r
            spread = jnp.where(own_block, query[pl.ds(b, 1), :cols], 0.0).astype(bf16)
            scores = lax.dot_general(
                spread, keys[b], (((1,), (1,)), ((), ())), preferred_element_type=f32
            )
            gate = gates[b]
            length = lengths[b]
            valid = place < length
            logits = scores * size ** (-0.5) - gate
            top = jnp.max(jnp.where(valid, logits, -1e30), axis=-1, keepdims=True)
            weights = jnp.where(valid, jnp.exp(logits - top), 0.0)
            total = jnp.sum(weights, axis=-1, keepdims=True)
            last = jnp.sum(jnp.where(place == length - 1, gate, 0.0), axis=-1, keepdims=True)
            summed = jnp.dot(weights.astype(bf16), values[b], preferred_element_type=f32)
            a_send[owner, r : r + 1, :cols] = jnp.sum(
                jnp.where(own_block, summed, 0.0), axis=0, keepdims=True
            )
            stats = jnp.where(
                stat_lane == stat_row,
                top,
                jnp.where(
                    stat_lane == stat_row + heads,
                    total,
                    jnp.where(stat_lane == stat_row + 2 * heads, last, 0.0),
                ),
            )
            a_send[owner, r : r + 1, cols:] = jnp.sum(stats, axis=0, keepdims=True)

    def attend_for(j, carry):
        attend(kv_peer(j))
        over_kv(2, j, lambda peer: a_send.at[peer], a_all).start()
        return carry

    lax.fori_loop(1, n_kv, attend_for, 0)
    attend(kv)
    a_all[kv] = a_send[kv]

    for j in range(1, n_kv):
        from_kv(1, j, lambda peer: p_send.at[peer], p_all)
    p_total = p_all[0]
    for o in range(1, n_kv):
        p_total = p_total + p_all[o]
    own_rows = [query[pl.ds(kv * mine + r, 1), :] for r in range(mine)]
    own_query = jnp.concatenate(own_rows, axis=0)
    own_scale = own_query[:, cols : cols + 1]
    own_query = own_query[:, :cols]
    new_key = (own_scale * p_total[:, :cols]).astype(bf16).astype(f32)
    new_value = (own_scale * p_total[:, cols : 2 * cols]).astype(bf16).astype(f32)
    gate_logit = own_scale * p_total[:, 2 * cols : 2 * cols + all_heads] + forget_bias[...]
    forget_log = jnp.minimum(gate_logit, 0.0) - jnp.log1p(jnp.exp(-jnp.abs(gate_logit)))
    col_head = lax.broadcasted_iota(jnp.int32, (mine, cols), 1) // size
    forget_wide = jnp.zeros((mine, cols), f32)
    for h in range(all_heads):
        forget_wide = jnp.where(col_head + tp * heads == h, forget_log[:, h : h + 1], forget_wide)
    product = own_query * new_key
    own = jnp.zeros((mine, cols), f32)
    for h in range(heads):
        inside = col_head == h
        own = jnp.where(
            inside, jnp.sum(jnp.where(inside, product, 0.0), axis=-1, keepdims=True), own
        )
    own = own * size ** (-0.5)

    for j in range(1, n_kv):
        from_kv(2, j, lambda peer: a_send.at[peer], a_all)

    def wide(part, first):
        result = jnp.zeros((mine, cols), f32)
        for h in range(heads):
            result = jnp.where(col_head == h, part[:, first + h : first + h + 1], result)
        return result

    tops = [wide(a_all[o, :, cols:], 0) for o in range(n_kv)]
    top = functools.reduce(jnp.maximum, tops)
    totals = jnp.zeros((mine, cols), f32)
    summed = jnp.zeros((mine, cols), f32)
    stat_sum = a_all[0, :, cols:]
    for o in range(1, n_kv):
        stat_sum = stat_sum + a_all[o, :, cols:]
    for o in range(n_kv):
        factor = jnp.exp(tops[o] - top)
        totals = totals + factor * wide(a_all[o, :, cols:], heads)
        summed = summed + factor * a_all[o, :, :cols]
    top = top + wide(stat_sum, 2 * heads) + forget_wide
    overall = jnp.maximum(top, own)
    cache_factor = jnp.exp(top - overall)
    own_weight = jnp.exp(own - overall)
    denominator = totals * cache_factor + own_weight
    numerator = summed * cache_factor + own_weight * new_value
    m_send[...] = (numerator / denominator).astype(bf16).astype(f32)
    for j in range(1, n_kv):
        send_kv(3, j, lambda peer: m_send, m_all)
    m_all[kv] = m_send[...]
    ld_o.wait()
    for j in range(1, n_kv):
        from_kv(3, j, lambda peer: m_send, m_all)
    for o in range(n_kv):
        mix[o * mine : (o + 1) * mine, :] = m_all[o]

    o_send[...] = jnp.dot(mix[...].astype(bf16), wo[...], preferred_element_type=f32).astype(bf16)
    for j in range(1, n_tp):
        send_tp(1, j, lambda peer: o_send, o_all)
    o_all[tp] = o_send[...]
    ld_u.wait()
    for j in range(1, n_tp):
        from_tp(1, j, lambda peer: o_send, o_all)
    attended = o_all[0].astype(f32)
    for t in range(1, n_tp):
        attended = attended + o_all[t].astype(f32)
    residual = (tok + attended).astype(bf16).astype(f32)
    for t in range(n_tp):
        res[t] = residual[:, t * piece : (t + 1) * piece]

    scaled_mid = (residual * gain_m).astype(bf16)
    share_squares(1, residual)

    def up_piece(owner):
        at = pl.multiple_of(owner * unit, unit)
        u_send[owner] = jnp.dot(
            scaled_mid, wu[:, pl.ds(at, unit)], preferred_element_type=f32
        ).astype(bf16)

    for j in range(1, n_kv):
        up_piece(kv_peer(j))
        send_kv(4, j, lambda peer: u_send.at[peer], u_all)
    up_piece(kv)
    u_all[kv] = u_send[kv]
    for j in range(1, n_kv):
        from_kv(4, j, lambda peer: u_send.at[peer], u_all)
    up_total = u_all[0].astype(f32)
    for o in range(1, n_kv):
        up_total = up_total + u_all[o].astype(f32)
    mixer_scale = lax.rsqrt(joined_squares(1) / width + norm_eps)
    active = jnp.maximum(mixer_scale * up_total, 0.0)
    h_send[...] = (active * active).astype(bf16)
    for j in range(1, n_kv):
        send_kv(5, j, lambda peer: h_send, h_all)

    ld_d.wait()

    def down_piece(block, owner):
        at = pl.multiple_of(owner * unit, unit)
        return jnp.dot(block, wd[pl.ds(at, unit), :], preferred_element_type=f32)

    down = down_piece(h_send[...], kv)
    for j in range(1, n_kv):
        peer = from_kv(5, j, lambda peer: h_send, h_all)
        down = down + down_piece(h_all[peer], peer)
    for t in range(n_tp):
        f_send[t] = down[:, t * piece : (t + 1) * piece]
    for j in range(1, n_tp):
        send_tp(2, j, lambda peer: f_send.at[peer], f_all)
    f_all[tp] = f_send[tp]
    for j in range(1, n_tp):
        from_tp(2, j, lambda peer: f_send.at[peer], f_all)
    mixer = f_all[0]
    for t in range(1, n_tp):
        mixer = mixer + f_all[t]
    out[...] = (res[tp] + mixer).astype(bf16)

    for copy in pending:
        copy.wait_send()
    for j in range(1, n_kv):
        over_kv(2, j, lambda peer: a_send.at[peer], a_all).wait_send()


def layer(n_kv, n_tp, *arrays):
    (
        tokens,
        gain_attn,
        w_query,
        w_key,
        w_value,
        w_forget,
        forget_bias,
        keys_cache,
        values_cache,
        gates_cache,
        lengths,
        w_out,
        gain_mixer,
        w_up,
        w_down,
    ) = arrays
    seqs, piece = tokens.shape
    rows, cols = w_query.shape
    heads = gates_cache.shape[1]
    all_heads = w_forget.shape[1]
    unit = w_up.shape[1] // n_kv
    fits = (
        piece % LANES == 0
        and cols % LANES == 0
        and unit % LANES == 0
        and seqs % n_kv == 0
        and 3 * heads <= LANES
        and all_heads < LANES
        and w_out.shape == (cols, rows)
        and seqs <= LANES
        and n_kv % 2 == 0
        and n_tp > 1
    )
    if not fits:
        return shards(*arrays)
    mine = seqs // n_kv
    vmem = pl.BlockSpec(memory_space=pltpu.VMEM)
    smem = pl.BlockSpec(memory_space=pltpu.SMEM)
    anywhere = pl.BlockSpec(memory_space=pl.ANY)

    def like(x):
        return pltpu.VMEM(x.shape, x.dtype)

    return pl.pallas_call(
        functools.partial(fused, n_kv, n_tp),
        out_shape=jax.ShapeDtypeStruct((seqs, piece), bf16),
        in_specs=[vmem, vmem, vmem, smem, vmem] + [anywhere] * 10,
        out_specs=vmem,
        scratch_shapes=[
            like(w_query),
            like(w_key),
            like(w_value),
            pltpu.VMEM((all_heads, rows), bf16),
            like(keys_cache),
            like(values_cache),
            like(gates_cache),
            like(w_out),
            like(w_up),
            like(w_down),
            pltpu.VMEM((n_tp, seqs, piece), bf16),
            pltpu.VMEM((seqs, cols), bf16),
            pltpu.VMEM((n_kv, seqs, cols), bf16),
            pltpu.VMEM((n_kv, mine, 2 * cols + LANES), f32),
            pltpu.VMEM((n_kv, mine, 2 * cols + LANES), f32),
            pltpu.VMEM((n_kv, mine, cols + LANES), f32),
            pltpu.VMEM((n_kv, mine, cols + LANES), f32),
            pltpu.VMEM((mine, cols), f32),
            pltpu.VMEM((n_kv, mine, cols), f32),
            pltpu.VMEM((seqs, rows), bf16),
            pltpu.VMEM((n_tp, seqs, rows), bf16),
            pltpu.VMEM((n_kv, seqs, unit), bf16),
            pltpu.VMEM((n_kv, seqs, unit), bf16),
            pltpu.VMEM((seqs, unit), bf16),
            pltpu.VMEM((n_kv, seqs, unit), bf16),
            pltpu.VMEM((n_tp, seqs, piece), f32),
            pltpu.VMEM((n_tp, seqs, piece), f32),
            pltpu.VMEM((seqs, cols + LANES), f32),
            pltpu.VMEM((seqs, cols), f32),
            pltpu.VMEM((n_tp, seqs, piece), f32),
            pltpu.VMEM((2, 1, LANES), f32),
            pltpu.VMEM((2, n_kv, 1, LANES), f32),
            pltpu.SemaphoreType.DMA((10,)),
            pltpu.SemaphoreType.DMA((8, n_kv)),
            pltpu.SemaphoreType.DMA((8, n_kv)),
            pltpu.SemaphoreType.DMA((3, n_tp)),
            pltpu.SemaphoreType.DMA((3, n_tp)),
        ],
        compiler_params=pltpu.CompilerParams(
            collective_id=0, has_side_effects=True, vmem_limit_bytes=60 * 1024 * 1024
        ),
    )(
        tokens,
        gain_attn,
        forget_bias.reshape(1, -1),
        lengths,
        gain_mixer,
        w_query,
        w_key,
        w_value,
        w_forget.T,
        keys_cache,
        values_cache,
        gates_cache,
        w_out,
        w_up,
        w_down,
    )


def solution(mesh):
    return jax.shard_map(
        functools.partial(layer, mesh.shape["kv"], mesh.shape["tp"]),
        mesh=mesh,
        in_specs=(
            P(None, ("kv", "tp")),
            P(),
            P("kv", "tp"),
            P("kv", "tp"),
            P("kv", "tp"),
            P(),
            P(),
            P(None, "kv", "tp"),
            P(None, "kv", "tp"),
            P(None, "tp", "kv"),
            P(),
            P("tp", "kv"),
            P(),
            P("kv", "tp"),
            P("tp", "kv"),
        ),
        out_specs=P(None, ("kv", "tp")),
        check_vma=False,
    )
```
